32 devices in a mesh: sp: 16 (over z, x, core), tp: 2 (over y).
Axes of the slice: x: 2, y: 2, z: 4, core: 2. Of those that a mesh axis runs over, the one named last changes fastest.
Arguments:
- linear_part: bfloat16 [32768, 2048], P('sp', 'tp'), may hold values from -6 to 6
- gate_part: bfloat16 [32768, 2048], P('sp', 'tp'), may hold values from -8 to 8
- kernel_taps: bfloat16 [31, 2048], P(None, 'tp'), may hold values from -10 to 10
- channel_gain: float32 [2048], replicated, may hold values from 0.1 to 1.9
- output_weight: bfloat16 [2048, 2048], P('tp'), may hold values from -0.125 to 0.125
- residual: bfloat16 [32768, 2048], P(('sp', 'tp')), may hold values from -6 to 6
- mix_gain: float32 [2048], replicated, may hold values from 0.1 to 1.9
- documents: int32 [32768], P('sp'), may hold values from 0 to 3, never falling along the last dimension, each value on 1 to 16384 neighbouring positions
- expert_ids: int32 [32768, 2], P(('sp', 'tp')), may hold values from 0 to 15, all different within a row; in each aligned block of 1024 rows (0 to 1023, 1024 to 2047, ...) at most 512 rows name the same one
- route_weights: float32 [32768, 2], P(('sp', 'tp')), may hold values from 0.25 to 2.5
- expert_gate: bfloat16 [16, 2048, 512], P('sp'), may hold values from -0.125 to 0.125
- expert_up: bfloat16 [16, 2048, 512], P('sp'), may hold values from -0.125 to 0.125
- expert_down: bfloat16 [16, 512, 2048], P('sp'), may hold values from -0.25 to 0.25
- shared_gate: bfloat16 [2048, 256], replicated, may hold values from -0.125 to 0.125
- shared_up: bfloat16 [2048, 256], replicated, may hold values from -0.125 to 0.125
- shared_down: bfloat16 [256, 2048], replicated, may hold values from -0.375 to 0.375
- final_gain: float32 [2048], replicated, may hold values from 0.1 to 1.9
Outputs:
- layer_out: bfloat16 [32768, 2048], P(('sp', 'tp'))
The draws below stay inside these ranges and needn't reach their ends.
Inputs may be any that keep to these rules, and one draw needn't show every extreme that they name: `expert_ids`: each row names 2 different experts; among the rows of one device (aligned blocks of 1024 rows) no expert is named by more than 512 rows, and exactly 512 in some block. `documents`: never falling along the sequence; each document 1 to 16384 positions.
All inputs are finite; a program needn't handle non-finite values.
Results may differ from the reference program's by a relative error of at most 0.0065.
Values may be sent and summed in bfloat16 or wider, within the bound.
A program may use at most 192 MiB of HBM per device.

```python
import math
import jax
import jax.numpy as jnp
import numpy as np
from jax import lax

D = 2048
KW = 31
FE = 512
FS = 256
TOP = 2
ROWS = 1024
TOKENS = 32768
EXPERTS = 16
CAP = 512
DOCS = 4
DOC_MOST = 16384
N_SP = 16
N_TP = 2


def draw_kernel_taps(key, part):
    first = jax.random.fold_in(key, 11)
    second = jax.random.fold_in(key, 12)
    base = jnp.clip(jax.random.normal(first, (KW, D), jnp.float32), -4.0, 4.0) / math.sqrt(KW)
    spread = 10.0 ** jax.random.uniform(second, (D,), jnp.float32)
    return (base * spread[None, :]).astype(jnp.bfloat16)


def steps_of(stream_key, dims, pieces, least, high):
    level = 1.0
    for axis_at, parts in pieces:
        heights = jax.random.uniform(jax.random.fold_in(jax.random.fold_in(stream_key, 6), axis_at), (parts,), jnp.float32, least / len(pieces), high / len(pieces))
        level = level * jnp.repeat(jnp.exp(heights), dims[axis_at] // parts).reshape((-1,) + (1,) * (len(dims) - 1 - axis_at))
    return level


def profile(count, total, most, slope):
    loads = [(1 << 20) // math.isqrt(standing ** slope) + 1 for standing in range(2, count + 1)]
    spare, counts = total - most - (count - 1), [1] * (count - 1)
    while spare > 0:
        free = [i for i in range(count - 1) if counts[i] < most]
        whole, budget = sum([loads[i] for i in free]), spare
        for i in free:
            extra = min(most - counts[i], max(1, budget * loads[i] // whole), spare)
            counts[i] = counts[i] + extra
            spare = spare - extra
    return np.array([most] + counts)


def uneven_parts(own_key, count, total, most, slope):
    if count == 2:
        one = jax.random.randint(own_key, (), max(1, total - most), min(most, total - 1) + 1)
        return jnp.stack([one, total - one])
    sizes = jnp.asarray(profile(count, total, most, slope), jnp.int32)
    twos = (count - 1) // 2
    source_of, taker = sizes[1:1 + 2 * twos:2], sizes[2:2 + 2 * twos:2]
    slack = jnp.minimum(source_of - 1, most - taker)
    passed = jax.random.randint(jax.random.fold_in(own_key, 1), (twos,), 0, 1 << 20) % (slack + 1)
    sizes = sizes.at[1:1 + 2 * twos:2].set(source_of - passed).at[2:2 + 2 * twos:2].set(taker + passed)
    return sizes[jax.random.permutation(jax.random.fold_in(own_key, 2), count)]


def assign_block(stream_key, own, number, rows, amount, top, most, skew):
    ranking = jax.random.permutation(stream_key, amount)
    packed, usual = shares(amount, rows * top, most, skew, True), shares(amount, rows * top, most, skew, False)
    places = jnp.arange(amount)

    def named(tallies, offset_by):
        used = int((tallies > 0).sum())
        fixed = max(1, used // 4)
        shifted = fixed + (places - fixed + offset_by * (used - fixed)) % max(1, amount - fixed)
        return jnp.zeros((amount,), jnp.int32).at[ranking[jnp.where(places < fixed, places, shifted)]].set(jnp.asarray(tallies, jnp.int32))

    tallies = jnp.where(number % 4 == 0, named(packed, number // 4), named(usual, number - number // 4 - 1))
    mixed = jax.random.permutation(jax.random.fold_in(own, 3), amount)
    giver, sink = mixed[0:amount // 2 * 2:2], mixed[1:amount // 2 * 2:2]
    margin = jnp.minimum(tallies[giver] - 1, most - tallies[sink]) // 2
    margin = jnp.where((giver == ranking[0]) | (sink == ranking[0]) | (tallies[sink] == 0), 0, jnp.maximum(margin, 0))
    shifted = jax.random.randint(jax.random.fold_in(own, 4), (amount // 2,), 0, 1 << 20) % (margin + 1)
    tallies = tallies.at[giver].add(-shifted).at[sink].add(shifted)
    labels = jnp.searchsorted(jnp.cumsum(tallies), jnp.arange(rows * top), side="right").astype(jnp.int32)
    grid = labels.reshape(top, rows).T
    grid = grid[jax.random.permutation(jax.random.fold_in(own, 1), rows)]
    offset_by = jax.random.randint(jax.random.fold_in(own, 2), (rows, 1), 0, top)
    return jnp.take_along_axis(grid, (jnp.arange(top)[None, :] + offset_by) % top, axis=1)


def shares(count, total, bound, skew, full):
    weights = [(1 << 20) // math.isqrt(rank ** skew) + 1 for rank in range(1, count + 1)]
    largest = bound if full else min(bound, max(-(-total // count), total * weights[0] // sum(weights)))
    least = 1 if total - largest >= count - 1 else 0
    holding, surplus = [largest] + [least] * (count - 1), total - largest - least * (count - 1)
    while surplus > 0:
        free = [i for i in range(1, count) if holding[i] < largest] or [i for i in range(1, count) if holding[i] < bound]
        whole, remaining = sum([weights[i] for i in free]), surplus
        for i in free:
            extra = min(bound - holding[i], max(1, remaining * weights[i] // whole), surplus)
            holding[i] = holding[i] + extra
            surplus = surplus - extra
    return np.array(holding)


def scatter_about(key, shape, width, most, split=(), kind=jnp.bfloat16):
    drawn = width * jax.random.normal(key, shape, jnp.float32)
    if split:
        drawn = drawn * steps_of(key, shape, split, -0.22, 0.18)
    return jnp.clip(drawn, -most, most).astype(kind)


def setup_inputs(seed: int = 0) -> dict:
    key_list = jax.random.split(jax.random.key(seed), 18)
    linear_part = scatter_about(key_list[0], (TOKENS, D), 1.0, 6.0, ((0, 16), (1, 2)))
    gate_part = scatter_about(key_list[1], (TOKENS, D), 1.5, 8.0, ((0, 16), (1, 2)))
    kernel_taps = draw_kernel_taps(jax.random.fold_in(key_list[17], 71), 0)
    channel_gain = jnp.clip(1.0 + 0.18 * jax.random.normal(key_list[3], (D,), jnp.float32), 0.1, 1.9)
    output_weight = scatter_about(key_list[4], (D, D), D ** -0.5, 0.125, ((0, 2),))
    residual = scatter_about(key_list[5], (TOKENS, D), 1.0, 6.0, ((0, 32),))
    mix_gain = jnp.clip(1.0 + 0.18 * jax.random.normal(key_list[6], (D,), jnp.float32), 0.1, 1.9)
    documents = jnp.searchsorted(jnp.cumsum(uneven_parts(key_list[7], DOCS, TOKENS, DOC_MOST, 2)), jnp.arange(TOKENS), side="right").astype(jnp.int32)
    expert_ids_keys = jax.random.split(jax.random.fold_in(key_list[8], 1), TOKENS // ROWS)
    expert_ids_turns = jax.random.permutation(jax.random.fold_in(key_list[8], 3), TOKENS // ROWS)
    expert_ids = jax.vmap(lambda own, number: assign_block(jax.random.fold_in(key_list[8], 2), own, number, ROWS, EXPERTS, TOP, CAP, 2))(expert_ids_keys, expert_ids_turns).reshape((TOKENS, TOP))
    route_weights = jnp.clip(jnp.exp(math.log(2.5) - 2.3025851 * jax.random.uniform(key_list[9], (TOKENS, TOP), jnp.float32) ** steps_of(key_list[9], (TOKENS, TOP), ((0, 32),), -0.2, 0.2)), 0.25, 2.5)
    expert_gate = scatter_about(key_list[10], (EXPERTS, D, FE), D ** -0.5, 0.125, ((0, 16),))
    expert_up = scatter_about(key_list[11], (EXPERTS, D, FE), D ** -0.5, 0.125, ((0, 16),))
    expert_down = scatter_about(key_list[12], (EXPERTS, FE, D), FE ** -0.5, 0.25, ((0, 16),))
    shared_gate = scatter_about(key_list[13], (D, FS), D ** -0.5, 0.125)
    shared_up = scatter_about(key_list[14], (D, FS), D ** -0.5, 0.125)
    shared_down = scatter_about(key_list[15], (FS, D), FS ** -0.5, 0.375)
    final_gain = jnp.clip(1.0 + 0.18 * jax.random.normal(key_list[16], (D,), jnp.float32), 0.1, 1.9)
    return {"linear_part": linear_part, "gate_part": gate_part, "kernel_taps": kernel_taps, "channel_gain": channel_gain, "output_weight": output_weight, "residual": residual, "mix_gain": mix_gain, "documents": documents, "expert_ids": expert_ids, "route_weights": route_weights, "expert_gate": expert_gate, "expert_up": expert_up, "expert_down": expert_down, "shared_gate": shared_gate, "shared_up": shared_up, "shared_down": shared_down, "final_gain": final_gain}


EPSILON = 1e-05
RESIDUAL_SCALE = 8.0 ** 0.25

def normalize(values):
    mean = lax.optimization_barrier(jnp.mean(values, -1, keepdims=True))
    square = lax.optimization_barrier(jnp.mean(values * values, -1, keepdims=True))
    return (values - mean) * lax.rsqrt(square - mean * mean + EPSILON)

def reference(linear_part, gate_part, kernel_taps, channel_gain, output_weight, residual, mix_gain, documents, expert_ids, route_weights, expert_gate, expert_up, expert_down, shared_gate, shared_up, shared_down, final_gain):
    gated = (linear_part.astype(jnp.float32) * jax.nn.sigmoid(gate_part.astype(jnp.float32))).astype(jnp.bfloat16)
    reach = KW - 1
    padded = jnp.concatenate([jnp.zeros((reach, D), jnp.bfloat16), gated], 0)
    padded_docs = jnp.concatenate([jnp.full((reach,), -1, jnp.int32), documents.astype(jnp.int32)], 0)
    taps = kernel_taps.astype(jnp.float32)
    total = jnp.zeros((TOKENS, D), jnp.float32)
    for offset in range(KW):
        window = padded[reach - offset:reach - offset + TOKENS].astype(jnp.float32)
        same = padded_docs[reach - offset:reach - offset + TOKENS] == documents.astype(jnp.int32)
        total = total + jnp.where(same[:, None], window * taps[offset], 0.0)
    convolved = total.astype(jnp.bfloat16)
    activated = jax.nn.silu(normalize(convolved.astype(jnp.float32)) * channel_gain).astype(jnp.bfloat16)
    projected = jnp.dot(activated, output_weight, preferred_element_type=jnp.float32)
    normed = (normalize(RESIDUAL_SCALE * residual.astype(jnp.float32) + projected) * mix_gain).astype(jnp.bfloat16)
    limit = N_SP * N_TP * CAP

    def visit(routed, inputs):
        gate_w, up_w, down_w, expert = inputs
        hits = expert_ids == expert
        named = jnp.any(hits, 1)
        where_rows = jnp.nonzero(named, size=limit, fill_value=0)[0].astype(jnp.int32)
        count = jnp.sum(named.astype(jnp.int32))
        live = jnp.arange(limit, dtype=jnp.int32) < count
        weight = lax.optimization_barrier(jnp.sum(jnp.where(hits, route_weights, 0.0), 1))[where_rows]
        weight = jnp.where(live, weight, 0.0)
        rows = normed[where_rows]
        hidden = (jax.nn.silu(jnp.dot(rows, gate_w, preferred_element_type=jnp.float32)) * jnp.dot(rows, up_w, preferred_element_type=jnp.float32)).astype(jnp.bfloat16)
        answer = jnp.dot(hidden, down_w, preferred_element_type=jnp.float32).astype(jnp.bfloat16)
        return (routed.at[where_rows].add(weight[:, None] * answer.astype(jnp.float32)), None)
    routed, _ = lax.scan(visit, jnp.zeros((TOKENS, D), jnp.float32), (expert_gate, expert_up, expert_down, jnp.arange(EXPERTS, dtype=jnp.int32)))
    common = (jax.nn.silu(jnp.dot(normed, shared_gate, preferred_element_type=jnp.float32)) * jnp.dot(normed, shared_up, preferred_element_type=jnp.float32)).astype(jnp.bfloat16)
    shared_out = jnp.dot(common, shared_down, preferred_element_type=jnp.float32)
    return (normalize(RESIDUAL_SCALE * normed.astype(jnp.float32) + routed + shared_out) * final_gain).astype(jnp.bfloat16)
```

```python
import functools

import jax
import jax.numpy as jnp
from jax import lax
from jax.experimental import pallas as pl
from jax.experimental.pallas import tpu as pltpu
from jax.sharding import PartitionSpec as P

EPSILON = 1e-05
RESIDUAL_SCALE = 8.0**0.25


def passed_along(block, axis, distance):
    devices = range(lax.axis_size(axis))
    route = [(i - distance, i) for i in devices if i - distance in devices]
    return lax.ppermute(block, axis, route)


def normalize(values):
    mean = jnp.mean(values, -1, keepdims=True)
    square = jnp.mean(values * values, -1, keepdims=True)
    return (values - mean) * lax.rsqrt(square - mean * mean + EPSILON)


def gathering_is_less(rows, chosen, experts_all, shape):
    weights = experts_all * 3 * shape[1] * shape[2]
    positions = 2 * experts_all * min(rows, 4 * rows * chosen // experts_all) * shape[1]
    return weights <= 2 * positions


def routed_by_weights(normed, expert_ids, route_weights, gates, ups, downs_first, downs_second):
    experts_all, half = downs_first.shape[:2]
    firsts, seconds = [], []
    for expert in range(experts_all):
        weight = jnp.sum(jnp.where(expert_ids == expert, route_weights, 0.0), 1, keepdims=True)
        hidden = jax.nn.silu(
            jnp.dot(normed, gates[expert], preferred_element_type=jnp.float32)
        ) * jnp.dot(normed, ups[expert], preferred_element_type=jnp.float32)
        weighted = (weight * hidden).astype(jnp.bfloat16)
        firsts.append(weighted[:, :half])
        seconds.append(weighted[:, half:])
    width = normed.shape[1]
    return jnp.dot(
        jnp.concatenate(firsts, 1),
        downs_first.reshape(experts_all * half, width),
        preferred_element_type=jnp.float32,
    ) + jnp.dot(
        jnp.concatenate(seconds, 1),
        downs_second.reshape(experts_all * half, width),
        preferred_element_type=jnp.float32,
    )


def routed_by_positions(normed, expert_ids, route_weights, expert_gate, expert_up, expert_down):
    rows = normed.shape[0]
    width_full = normed.shape[1]
    chosen = expert_ids.shape[1]
    experts_all = lax.axis_size("sp") * expert_gate.shape[0]
    capacity = min(rows, 4 * rows * chosen // experts_all)
    flat_ids = expert_ids.reshape(-1)
    onehot = (flat_ids[:, None] == jnp.arange(experts_all, dtype=jnp.int32)[None, :]).astype(
        jnp.int32
    )
    earlier = jnp.cumsum(onehot, 0) - onehot
    ranks = jnp.sum(earlier * onehot, 1)
    slots = flat_ids * capacity + ranks
    places = jnp.arange(experts_all * capacity, dtype=jnp.int32)[:, None] == slots[None, :]
    chooser = jnp.any(places.reshape(experts_all * capacity, rows, chosen), 2).astype(jnp.bfloat16)
    outgoing = jnp.dot(chooser, normed, preferred_element_type=jnp.float32).astype(jnp.bfloat16)
    outgoing = outgoing.reshape(experts_all, capacity, width_full)
    arrived = lax.all_to_all(outgoing, "sp", split_axis=0, concat_axis=0, tiled=True)
    sources, items, width = arrived.shape
    flat = arrived.reshape(sources * items, width)
    hidden = (
        jax.nn.silu(jnp.dot(flat, expert_gate[0], preferred_element_type=jnp.float32))
        * jnp.dot(flat, expert_up[0], preferred_element_type=jnp.float32)
    ).astype(jnp.bfloat16)
    answer = jnp.dot(hidden, expert_down[0], preferred_element_type=jnp.float32).astype(
        jnp.bfloat16
    )
    answered = answer.reshape(sources, items, width)
    returned = lax.all_to_all(answered, "sp", split_axis=0, concat_axis=0, tiled=True).reshape(
        experts_all * capacity, width_full
    )
    picked = jnp.take(returned, slots, axis=0).astype(jnp.float32).reshape(rows, chosen, width_full)
    return jnp.sum(picked * route_weights[:, :, None], 1)


def shards_any(
    linear_part,
    gate_part,
    kernel_taps,
    channel_gain,
    output_weight,
    residual,
    mix_gain,
    documents,
    expert_ids,
    route_weights,
    expert_gate,
    expert_up,
    expert_down,
    shared_gate,
    shared_up,
    shared_down,
    final_gain,
):
    experts_all = lax.axis_size("sp") * expert_gate.shape[0]
    gathers = gathering_is_less(residual.shape[0], expert_ids.shape[1], experts_all, expert_gate.shape)
    weight_all = lax.all_gather(output_weight, "tp", axis=0, tiled=True)
    if gathers:
        half = expert_down.shape[1] // 2
        weight_all, expert_gate, expert_up, first, second = lax.optimization_barrier(
            (weight_all, expert_gate, expert_up, expert_down[:, :half], expert_down[:, half:])
        )
        gates, ups, downs_first, downs_second = [
            lax.all_gather(part, "sp", axis=0, tiled=True)
            for part in (expert_gate, expert_up, first, second)
        ]
    reach = kernel_taps.shape[0] - 1
    length = linear_part.shape[0]
    gated = (
        linear_part.astype(jnp.float32) * jax.nn.sigmoid(gate_part.astype(jnp.float32))
    ).astype(jnp.bfloat16)
    before, before_docs = passed_along(
        (gated[length - reach :], documents[length - reach :]), "sp", 1
    )
    extended = jnp.concatenate([before, gated], 0)
    extended_docs = jnp.concatenate([before_docs, documents], 0)
    taps = kernel_taps.astype(jnp.float32)
    total = jnp.zeros(gated.shape, jnp.float32)
    for offset in range(reach + 1):
        window = lax.slice_in_dim(extended, reach - offset, reach - offset + length, axis=0).astype(
            jnp.float32
        )
        same = (
            lax.slice_in_dim(extended_docs, reach - offset, reach - offset + length, axis=0)
            == documents
        )
        total = total + jnp.where(same[:, None], window * taps[offset], 0.0)
    convolved = total.astype(jnp.bfloat16)
    position_rows = lax.all_to_all(convolved, "tp", split_axis=0, concat_axis=1, tiled=True)
    activated = jax.nn.silu(normalize(position_rows.astype(jnp.float32)) * channel_gain).astype(
        jnp.bfloat16
    )
    projected = jnp.dot(
        activated,
        weight_all,
        preferred_element_type=jnp.float32,
    )
    normed = (
        normalize(RESIDUAL_SCALE * residual.astype(jnp.float32) + projected) * mix_gain
    ).astype(jnp.bfloat16)
    if gathers:
        routed = routed_by_weights(
            normed, expert_ids, route_weights, gates, ups, downs_first, downs_second
        )
    else:
        routed = routed_by_positions(
            normed, expert_ids, route_weights, expert_gate, expert_up, expert_down
        )
    common = (
        jax.nn.silu(jnp.dot(normed, shared_gate, preferred_element_type=jnp.float32))
        * jnp.dot(normed, shared_up, preferred_element_type=jnp.float32)
    ).astype(jnp.bfloat16)
    shared_out = jnp.dot(common, shared_down, preferred_element_type=jnp.float32)
    return (
        normalize(RESIDUAL_SCALE * normed.astype(jnp.float32) + routed + shared_out) * final_gain
    ).astype(jnp.bfloat16)


HALO = 32
LANES = 128
PIECE = 128


def column_of(table, lane):
    lanes = lax.broadcasted_iota(jnp.int32, table.shape, 1)
    return jnp.sum(jnp.where(lanes == lane, table, 0.0), 1, keepdims=True)


def conv_kernel(taps, part_ref, lin_ref, gate_ref, lin_back_ref, gate_back_ref, halo_ref, tap_ref, runs_ref, short_ref, out_ref, held):
    rows = out_ref.shape[0]

    def gated_of(lin, gate):
        lin = lin.astype(jnp.float32)
        gate = gate.astype(jnp.float32)
        return (lin * jax.nn.sigmoid(gate)).astype(jnp.bfloat16).astype(jnp.float32)

    @pl.when(part_ref[0] == 0)
    def _():
        held[0:HALO] = halo_ref[...].astype(jnp.float32)

    @pl.when(part_ref[0] != 0)
    def _():
        held[0:HALO] = gated_of(lin_back_ref[...], gate_back_ref[...])

    @pl.loop(0, rows // LANES)
    def _(i):
        at = pl.multiple_of(i * LANES, LANES)
        held[pl.ds(pl.multiple_of(HALO + at, HALO), LANES)] = gated_of(
            lin_ref[pl.ds(at, LANES)], gate_ref[pl.ds(at, LANES)]
        )

    step = 64

    @pl.loop(0, rows // step)
    def _(i):
        at = pl.multiple_of(i * step, step)

        def summed(masked):
            total = jnp.zeros((step, LANES), jnp.float32)
            run = runs_ref[pl.ds(at, step)] if masked else None
            for offset in range(taps):
                window = held[pl.ds(at + (HALO - offset), step)]
                term = window * tap_ref[offset : offset + 1]
                if masked:
                    term = jnp.where(run >= offset, term, 0.0)
                total = total + term
            out_ref[pl.ds(at, step)] = total.astype(out_ref.dtype)

        short = short_ref[i] != 0

        @pl.when(short)
        def _():
            summed(True)

        @pl.when(jnp.logical_not(short))
        def _():
            summed(False)


def convolve(part, linear_part, gate_part, halo, taps, runs, short):
    rows = linear_part.shape[0] // 2
    width = linear_part.shape[1]
    back = rows // HALO
    block = lambda of: pl.BlockSpec((rows, LANES), of)
    return pl.pallas_call(
        functools.partial(conv_kernel, taps.shape[0]),
        out_shape=jax.ShapeDtypeStruct((rows, width), jnp.bfloat16),
        grid_spec=pltpu.PrefetchScalarGridSpec(
            num_scalar_prefetch=1,
            grid=(width // LANES,),
            in_specs=[
                block(lambda c, part: (part[0], c)),
                block(lambda c, part: (part[0], c)),
                pl.BlockSpec((HALO, LANES), lambda c, part: (part[0] * back - part[0], c)),
                pl.BlockSpec((HALO, LANES), lambda c, part: (part[0] * back - part[0], c)),
                pl.BlockSpec((HALO, LANES), lambda c, part: (0, c)),
                pl.BlockSpec((taps.shape[0], LANES), lambda c, part: (0, c)),
                block(lambda c, part: (0, 0)),
                pl.BlockSpec(memory_space=pltpu.SMEM),
            ],
            out_specs=block(lambda c, part: (0, c)),
            scratch_shapes=[pltpu.VMEM((HALO + rows, LANES), jnp.float32)],
        ),
        cost_estimate=pl.CostEstimate(
            flops=rows * width * taps.shape[0] * 12, bytes_accessed=rows * width * 6, transcendentals=0
        ),
        compiler_params=pltpu.CompilerParams(dimension_semantics=("arbitrary",)),
        name="convolve",
    )(part, linear_part, gate_part, linear_part, gate_part, halo, taps, runs, short)


def row_norm(values):
    width = values.shape[1]
    mean = jnp.sum(values, 1, keepdims=True) * (1.0 / width)
    square = jnp.sum(values * values, 1, keepdims=True) * (1.0 / width)
    return (values - mean) * lax.rsqrt(square - mean * mean + EPSILON)


def project_kernel(own_ref, came_ref, own_gain_ref, came_gain_ref, w_own_ref, w_came_ref, residual_ref, gain_ref, *refs):
    out_ref = refs[-1]
    own = own_ref[...].astype(jnp.float32)
    came = came_ref[...].astype(jnp.float32)
    width = own.shape[1] + came.shape[1]
    mean = (jnp.sum(own, 1, keepdims=True) + jnp.sum(came, 1, keepdims=True)) * (1.0 / width)
    square = (
        jnp.sum(own * own, 1, keepdims=True) + jnp.sum(came * came, 1, keepdims=True)
    ) * (1.0 / width)
    scale = lax.rsqrt(square - mean * mean + EPSILON)
    own = jax.nn.silu((own - mean) * scale * own_gain_ref[...]).astype(jnp.bfloat16)
    came = jax.nn.silu((came - mean) * scale * came_gain_ref[...]).astype(jnp.bfloat16)
    projected = jnp.dot(own, w_own_ref[...], preferred_element_type=jnp.float32) + jnp.dot(
        came, w_came_ref[...], preferred_element_type=jnp.float32
    )
    mixed = RESIDUAL_SCALE * residual_ref[...].astype(jnp.float32) + projected
    out_ref[...] = (row_norm(mixed) * gain_ref[...]).astype(out_ref.dtype)


def project(first, count, own, came, own_gain, came_gain, w_own, w_came, residual, gain, before):
    total_rows, width = residual.shape
    half = own.shape[1]
    rows = min(count, 256)
    start = first // rows
    whole = lambda shape: pl.BlockSpec(shape, lambda r: (0, 0))
    here = lambda columns: pl.BlockSpec((rows, columns), lambda r: (r + start, 0))
    in_specs = [
        here(half),
        here(half),
        whole((1, half)),
        whole((1, half)),
        whole((half, width)),
        whole((half, width)),
        here(width),
        whole((1, width)),
    ]
    operands = [own, came, own_gain, came_gain, w_own, w_came, residual, gain]
    if before is not None:
        in_specs.append(pl.BlockSpec(memory_space=pl.ANY))
        operands.append(before)
    return pl.pallas_call(
        project_kernel,
        out_shape=jax.ShapeDtypeStruct((total_rows, width), jnp.bfloat16),
        grid=(count // rows,),
        in_specs=in_specs,
        out_specs=here(width),
        input_output_aliases={} if before is None else {8: 0},
        cost_estimate=pl.CostEstimate(
            flops=2 * count * width * width, bytes_accessed=4 * half * width + 6 * count * width, transcendentals=0
        ),
        compiler_params=pltpu.CompilerParams(dimension_semantics=("arbitrary",)),
        name="project",
    )(*operands)


def experts_kernel(group, piece, has_start, later, start_at, x_ref, table_ref, w_ref, *refs):
    start_ref = refs[0] if has_start else None
    out_ref, total, in_sem, out_sem = refs[has_start + later :]
    rows, width = x_ref.shape
    step = pl.program_id(0)
    last = pl.num_programs(0) - 1
    tile = min(rows, 512)
    wide = 2 * piece

    @pl.when(step == 0)
    def _():
        if has_start:
            copy = pltpu.make_async_copy(start_ref.at[pl.ds(start_at, rows)], total, in_sem)
            copy.start()
            copy.wait()
        else:
            total[...] = jnp.zeros_like(total)

    @pl.loop(0, rows // tile)
    def _(i):
        at = pl.ds(pl.multiple_of(i * tile, tile), tile)
        x = x_ref[at]
        table = table_ref[at]
        hidden = []
        for member in range(group):
            both = jnp.dot(x, w_ref[member, :width], preferred_element_type=jnp.float32)
            gate, up = both[:, :piece], both[:, piece:]
            weight = column_of(table, step * group + member)
            hidden.append((jax.nn.silu(gate) * up * weight).astype(jnp.bfloat16))
        hidden = jnp.concatenate(hidden, 1)
        for block in range(width // wide):
            low = width + block * piece
            down = jnp.concatenate([w_ref[member, low : low + piece] for member in range(group)], 0)
            columns = slice(block * wide, (block + 1) * wide)
            total[at, columns] += jnp.dot(hidden, down, preferred_element_type=jnp.float32)

    @pl.when(step == last)
    def _():
        if out_ref.dtype == jnp.float32:
            copy = pltpu.make_async_copy(total, out_ref, out_sem)
            copy.start()
            copy.wait()
        else:
            out_ref[...] = total[...].astype(out_ref.dtype)


def experts(at, x, table, weights, start, dtype, after=()):
    first, count = at
    width = x.shape[1]
    experts_all, depth, wide = weights.shape
    piece = wide // 2
    group = 4 if experts_all % 4 == 0 else experts_all
    here = first // count
    anywhere = pl.BlockSpec(memory_space=pl.ANY)
    in_specs = [
        pl.BlockSpec((count, width), lambda e: (here, 0)),
        pl.BlockSpec((count, LANES), lambda e: (here, 0)),
        pl.BlockSpec((group, depth, wide), lambda e: (e, 0, 0)),
    ]
    operands = [x, table, weights]
    if start is not None:
        operands.append(start)
    operands.extend(after)
    in_specs.extend([anywhere] * (len(operands) - 3))
    kept = dtype == jnp.float32
    return pl.pallas_call(
        functools.partial(experts_kernel, group, piece, start is not None, len(after), first),
        out_shape=jax.ShapeDtypeStruct((count, width), dtype),
        grid=(experts_all // group,),
        in_specs=in_specs,
        out_specs=anywhere if kept else pl.BlockSpec((count, width), lambda e: (0, 0)),
        scratch_shapes=[
            pltpu.VMEM((count, width), jnp.float32),
            pltpu.SemaphoreType.DMA,
            pltpu.SemaphoreType.DMA,
        ],
        cost_estimate=pl.CostEstimate(
            flops=2 * count * experts_all * depth * wide,
            bytes_accessed=2 * experts_all * depth * wide + 8 * count * width,
            transcendentals=0,
        ),
        compiler_params=pltpu.CompilerParams(
            dimension_semantics=("arbitrary",), vmem_limit_bytes=56 * 1024 * 1024
        ),
        name="experts",
    )(*operands)


def finish_kernel(normed_ref, routed_ref, shared_ref, came_ref, gain_ref, *refs):
    mixed = RESIDUAL_SCALE * normed_ref[...].astype(jnp.float32) + routed_ref[...]
    mixed = mixed + shared_ref[...] + came_ref[...].astype(jnp.float32)
    refs[-1][...] = (row_norm(mixed) * gain_ref[...]).astype(jnp.bfloat16)


def finish(first, normed, routed, shared, came, gain, before):
    rows, width = normed.shape
    count = came.shape[0]
    tile = 128
    start = first // tile
    here = pl.BlockSpec((tile, width), lambda r: (r + start, 0))
    in_specs = [here, here, here, pl.BlockSpec((tile, width), lambda r: (r, 0)), pl.BlockSpec((1, width), lambda r: (0, 0))]
    operands = [normed, routed, shared, came, gain]
    if before is not None:
        in_specs.append(pl.BlockSpec(memory_space=pl.ANY))
        operands.append(before)
    return pl.pallas_call(
        finish_kernel,
        out_shape=jax.ShapeDtypeStruct((rows, width), jnp.bfloat16),
        grid=(count // tile,),
        in_specs=in_specs,
        out_specs=here,
        input_output_aliases={} if before is None else {5: 0},
        cost_estimate=pl.CostEstimate(
            flops=10 * count * width, bytes_accessed=14 * count * width, transcendentals=0
        ),
        compiler_params=pltpu.CompilerParams(dimension_semantics=("arbitrary",)),
        name="finish",
    )(*operands)


def packed(gate, up, down, low):
    width = gate.shape[0]
    blocks = width // (2 * PIECE)
    both = jnp.concatenate(
        [lax.dynamic_slice_in_dim(gate, low, PIECE, 1), lax.dynamic_slice_in_dim(up, low, PIECE, 1)], 1
    )
    below = lax.dynamic_slice_in_dim(down, low, PIECE, 0)
    below = below.reshape(PIECE, blocks, 2 * PIECE).transpose(1, 0, 2).reshape(blocks * PIECE, 2 * PIECE)
    return jnp.concatenate([both, below], 0)[None]


def swapped(block, axis):
    return lax.ppermute(block, axis, [(i, i ^ 1) for i in range(lax.axis_size(axis))])


def weight_table(names, weights):
    lanes = jnp.arange(LANES, dtype=jnp.float32)[None, :]
    return sum(
        jnp.where(names[k][:, None] == lanes, weights[k][:, None], 0.0) for k in range(names.shape[0])
    )


def shards_split(
    linear_part,
    gate_part,
    kernel_taps,
    channel_gain,
    output_weight,
    residual,
    mix_gain,
    documents,
    expert_ids,
    route_weights,
    expert_gate,
    expert_up,
    expert_down,
    shared_gate,
    shared_up,
    shared_down,
    final_gain,
):
    mine = lax.axis_index("tp")
    other = 1 - mine
    reach = kernel_taps.shape[0] - 1
    length = linear_part.shape[0]
    rows, width = residual.shape
    half = width // 2
    chosen = expert_ids.shape[1]
    low = mine * (expert_gate.shape[2] // 2)

    pieces = [
        packed(expert_gate[0], expert_up[0], expert_down[0], low + at)
        for at in range(0, expert_gate.shape[2] // 2, PIECE)
    ]
    gathered = [lax.all_gather(piece, "sp", axis=0, tiled=True) for piece in pieces]

    last_gated = (
        linear_part[length - HALO :].astype(jnp.float32)
        * jax.nn.sigmoid(gate_part[length - HALO :].astype(jnp.float32))
    ).astype(jnp.bfloat16)
    halo, halo_docs = passed_along((last_gated, documents[length - reach :]), "sp", 1)
    docs = jnp.concatenate([halo_docs, documents], 0)
    runs = sum(
        (docs[reach - offset : reach - offset + length] == documents).astype(jnp.int32)
        for offset in range(1, reach + 1)
    )
    short = (jnp.min(runs.reshape(length // 64, 64), 1) < reach).astype(jnp.int32)
    taps = kernel_taps.astype(jnp.float32)

    def conv_of(part):
        own_runs = lax.dynamic_slice_in_dim(runs, part * rows, rows)
        own_short = lax.dynamic_slice_in_dim(short, part * (rows // 64), rows // 64)
        return convolve(
            part[None],
            linear_part,
            gate_part,
            halo,
            taps,
            jnp.broadcast_to(own_runs[:, None], (rows, LANES)),
            own_short,
        )

    odd = lax.axis_index("sp") % 2
    quarter = half // 2
    fetched = swapped(lax.dynamic_slice_in_dim(output_weight, odd * quarter, quarter, 0), "tp")
    theirs = conv_of(other)
    came = swapped(theirs, "tp")
    own = conv_of(mine)
    fetched, own = lax.optimization_barrier((fetched, own))
    beside = swapped(fetched, "sp")
    w_came = jnp.concatenate([jnp.where(odd == 0, fetched, beside), jnp.where(odd == 0, beside, fetched)], 0)

    gain = channel_gain[None, :]
    own_gain = lax.dynamic_slice_in_dim(gain, mine * half, half, 1)
    came_gain = lax.dynamic_slice_in_dim(gain, other * half, half, 1)
    named = jnp.concatenate([expert_ids.T.astype(jnp.float32), route_weights.T], 0)
    named_there = swapped(named, "tp")
    table = weight_table(named[:chosen], named[chosen:])
    table_there = weight_table(named_there[:chosen], named_there[chosen:])

    part = rows // 2
    gains = mix_gain[None, :]
    normed, there = None, []
    for at in (0, part):
        normed = project(
            at, part, own, came, own_gain, came_gain, output_weight, w_came, residual, gains, normed
        )
        there.append(swapped(lax.slice_in_dim(normed, at, at + part), "tp"))

    common = (
        jax.nn.silu(jnp.dot(normed, shared_gate, preferred_element_type=jnp.float32))
        * jnp.dot(normed, shared_up, preferred_element_type=jnp.float32)
    ).astype(jnp.bfloat16)
    shared_out = jnp.dot(common, shared_down, preferred_element_type=jnp.float32)

    here_sum = experts((0, rows), normed, table, gathered[0], None, jnp.float32)
    there_sums = [
        experts((0, part), there[k], table_there[k * part : (k + 1) * part], gathered[0], None, jnp.float32, (here_sum,))
        for k in range(2)
    ]
    waited = (here_sum, *there_sums)
    returned = []
    for first, count in ((0, part // 2), (part // 2, part // 2), (part, part)):
        k, at = divmod(first, part)
        done = experts(
            (at, count),
            there[k],
            table_there[k * part : (k + 1) * part],
            gathered[1],
            there_sums[k],
            jnp.bfloat16,
            waited,
        )
        returned.append(swapped(done, "tp"))
    routed = experts((0, rows), normed, table, gathered[1], here_sum, jnp.float32, waited)
    out, at = None, 0
    for block in returned:
        out = finish(at, normed, routed, shared_out, block, final_gain[None, :], out)
        at += block.shape[0]
    return out


def shards(*arguments):
    linear_part, kernel_taps, residual, expert_gate = [arguments[at] for at in (0, 2, 5, 10)]
    splits = (
        lax.axis_size("tp") == 2
        and lax.axis_size("sp") % 4 == 0
        and expert_gate.shape[0] == 1
        and expert_gate.shape[2] == 4 * PIECE
        and residual.shape[0] % 1024 == 0
        and residual.shape[1] % 1024 == 0
        and kernel_taps.shape[0] <= HALO
    )
    return shards_split(*arguments) if splits else shards_any(*arguments)


def solution(mesh):
    return jax.shard_map(
        shards,
        mesh=mesh,
        in_specs=(
            P("sp", "tp"),
            P("sp", "tp"),
            P(None, "tp"),
            P(),
            P("tp", None),
            P(("sp", "tp"), None),
            P(),
            P("sp"),
            P(("sp", "tp"), None),
            P(("sp", "tp"), None),
            P("sp", None, None),
            P("sp", None, None),
            P("sp", None, None),
            P(),
            P(),
            P(),
            P(),
        ),
        out_specs=P(("sp", "tp"), None),
        check_vma=False,
    )
```

```python
import functools

import jax
import jax.numpy as jnp
from jax import lax
from jax.experimental import pallas as pl
from jax.experimental.pallas import tpu as pltpu
from jax.sharding import PartitionSpec as P

EPSILON = 1e-05
RESIDUAL_SCALE = 8.0**0.25


def passed_along(block, axis, distance):
    devices = range(lax.axis_size(axis))
    route = [(i - distance, i) for i in devices if i - distance in devices]
    return lax.ppermute(block, axis, route)


def normalize(values):
    mean = jnp.mean(values, -1, keepdims=True)
    square = jnp.mean(values * values, -1, keepdims=True)
    return (values - mean) * lax.rsqrt(square - mean * mean + EPSILON)


def gathering_is_less(rows, chosen, experts_all, shape):
    weights = experts_all * 3 * shape[1] * shape[2]
    positions = 2 * experts_all * min(rows, 4 * rows * chosen // experts_all) * shape[1]
    return weights <= 2 * positions


def routed_by_weights(normed, expert_ids, route_weights, gates, ups, downs_first, downs_second):
    experts_all, half = downs_first.shape[:2]
    firsts, seconds = [], []
    for expert in range(experts_all):
        weight = jnp.sum(jnp.where(expert_ids == expert, route_weights, 0.0), 1, keepdims=True)
        hidden = jax.nn.silu(
            jnp.dot(normed, gates[expert], preferred_element_type=jnp.float32)
        ) * jnp.dot(normed, ups[expert], preferred_element_type=jnp.float32)
        weighted = (weight * hidden).astype(jnp.bfloat16)
        firsts.append(weighted[:, :half])
        seconds.append(weighted[:, half:])
    width = normed.shape[1]
    return jnp.dot(
        jnp.concatenate(firsts, 1),
        downs_first.reshape(experts_all * half, width),
        preferred_element_type=jnp.float32,
    ) + jnp.dot(
        jnp.concatenate(seconds, 1),
        downs_second.reshape(experts_all * half, width),
        preferred_element_type=jnp.float32,
    )


def routed_by_positions(normed, expert_ids, route_weights, expert_gate, expert_up, expert_down):
    rows = normed.shape[0]
    width_full = normed.shape[1]
    chosen = expert_ids.shape[1]
    experts_all = lax.axis_size("sp") * expert_gate.shape[0]
    capacity = min(rows, 4 * rows * chosen // experts_all)
    flat_ids = expert_ids.reshape(-1)
    onehot = (flat_ids[:, None] == jnp.arange(experts_all, dtype=jnp.int32)[None, :]).astype(
        jnp.int32
    )
    earlier = jnp.cumsum(onehot, 0) - onehot
    ranks = jnp.sum(earlier * onehot, 1)
    slots = flat_ids * capacity + ranks
    places = jnp.arange(experts_all * capacity, dtype=jnp.int32)[:, None] == slots[None, :]
    chooser = jnp.any(places.reshape(experts_all * capacity, rows, chosen), 2).astype(jnp.bfloat16)
    outgoing = jnp.dot(chooser, normed, preferred_element_type=jnp.float32).astype(jnp.bfloat16)
    outgoing = outgoing.reshape(experts_all, capacity, width_full)
    arrived = lax.all_to_all(outgoing, "sp", split_axis=0, concat_axis=0, tiled=True)
    sources, items, width = arrived.shape
    flat = arrived.reshape(sources * items, width)
    hidden = (
        jax.nn.silu(jnp.dot(flat, expert_gate[0], preferred_element_type=jnp.float32))
        * jnp.dot(flat, expert_up[0], preferred_element_type=jnp.float32)
    ).astype(jnp.bfloat16)
    answer = jnp.dot(hidden, expert_down[0], preferred_element_type=jnp.float32).astype(
        jnp.bfloat16
    )
    answered = answer.reshape(sources, items, width)
    returned = lax.all_to_all(answered, "sp", split_axis=0, concat_axis=0, tiled=True).reshape(
        experts_all * capacity, width_full
    )
    picked = jnp.take(returned, slots, axis=0).astype(jnp.float32).reshape(rows, chosen, width_full)
    return jnp.sum(picked * route_weights[:, :, None], 1)


def shards_any(
    linear_part,
    gate_part,
    kernel_taps,
    channel_gain,
    output_weight,
    residual,
    mix_gain,
    documents,
    expert_ids,
    route_weights,
    expert_gate,
    expert_up,
    expert_down,
    shared_gate,
    shared_up,
    shared_down,
    final_gain,
):
    experts_all = lax.axis_size("sp") * expert_gate.shape[0]
    gathers = gathering_is_less(residual.shape[0], expert_ids.shape[1], experts_all, expert_gate.shape)
    weight_all = lax.all_gather(output_weight, "tp", axis=0, tiled=True)
    if gathers:
        half = expert_down.shape[1] // 2
        weight_all, expert_gate, expert_up, first, second = lax.optimization_barrier(
            (weight_all, expert_gate, expert_up, expert_down[:, :half], expert_down[:, half:])
        )
        gates, ups, downs_first, downs_second = [
            lax.all_gather(part, "sp", axis=0, tiled=True)
            for part in (expert_gate, expert_up, first, second)
        ]
    reach = kernel_taps.shape[0] - 1
    length = linear_part.shape[0]
    gated = (
        linear_part.astype(jnp.float32) * jax.nn.sigmoid(gate_part.astype(jnp.float32))
    ).astype(jnp.bfloat16)
    before, before_docs = passed_along(
        (gated[length - reach :], documents[length - reach :]), "sp", 1
    )
    extended = jnp.concatenate([before, gated], 0)
    extended_docs = jnp.concatenate([before_docs, documents], 0)
    taps = kernel_taps.astype(jnp.float32)
    total = jnp.zeros(gated.shape, jnp.float32)
    for offset in range(reach + 1):
        window = lax.slice_in_dim(extended, reach - offset, reach - offset + length, axis=0).astype(
            jnp.float32
        )
        same = (
            lax.slice_in_dim(extended_docs, reach - offset, reach - offset + length, axis=0)
            == documents
        )
        total = total + jnp.where(same[:, None], window * taps[offset], 0.0)
    convolved = total.astype(jnp.bfloat16)
    position_rows = lax.all_to_all(convolved, "tp", split_axis=0, concat_axis=1, tiled=True)
    activated = jax.nn.silu(normalize(position_rows.astype(jnp.float32)) * channel_gain).astype(
        jnp.bfloat16
    )
    projected = jnp.dot(
        activated,
        weight_all,
        preferred_element_type=jnp.float32,
    )
    normed = (
        normalize(RESIDUAL_SCALE * residual.astype(jnp.float32) + projected) * mix_gain
    ).astype(jnp.bfloat16)
    if gathers:
        routed = routed_by_weights(
            normed, expert_ids, route_weights, gates, ups, downs_first, downs_second
        )
    else:
        routed = routed_by_positions(
            normed, expert_ids, route_weights, expert_gate, expert_up, expert_down
        )
    common = (
        jax.nn.silu(jnp.dot(normed, shared_gate, preferred_element_type=jnp.float32))
        * jnp.dot(normed, shared_up, preferred_element_type=jnp.float32)
    ).astype(jnp.bfloat16)
    shared_out = jnp.dot(common, shared_down, preferred_element_type=jnp.float32)
    return (
        normalize(RESIDUAL_SCALE * normed.astype(jnp.float32) + routed + shared_out) * final_gain
    ).astype(jnp.bfloat16)


HALO = 32
LANES = 128
PIECE = 128


def column_of(table, lane):
    lanes = lax.broadcasted_iota(jnp.int32, table.shape, 1)
    return jnp.sum(jnp.where(lanes == lane, table, 0.0), 1, keepdims=True)


def conv_kernel(taps, part_ref, lin_ref, gate_ref, lin_back_ref, gate_back_ref, halo_ref, tap_ref, runs_ref, short_ref, *refs):
    out_ref, held = refs[-2:]
    rows = out_ref.shape[0]

    def gated_of(lin, gate):
        lin = lin.astype(jnp.float32)
        gate = gate.astype(jnp.float32)
        return (lin * jax.nn.sigmoid(gate)).astype(jnp.bfloat16).astype(jnp.float32)

    @pl.when(part_ref[0] == 0)
    def _():
        held[0:HALO] = halo_ref[...].astype(jnp.float32)

    @pl.when(part_ref[0] != 0)
    def _():
        held[0:HALO] = gated_of(lin_back_ref[...], gate_back_ref[...])

    @pl.loop(0, rows // LANES)
    def _(i):
        at = pl.multiple_of(i * LANES, LANES)
        held[pl.ds(pl.multiple_of(HALO + at, HALO), LANES)] = gated_of(
            lin_ref[pl.ds(at, LANES)], gate_ref[pl.ds(at, LANES)]
        )

    step = 64

    @pl.loop(0, rows // step)
    def _(i):
        at = pl.multiple_of(i * step, step)

        def summed(masked):
            total = jnp.zeros((step, LANES), jnp.float32)
            run = runs_ref[pl.ds(at, step)] if masked else None
            for offset in range(taps):
                window = held[pl.ds(at + (HALO - offset), step)]
                term = window * tap_ref[offset : offset + 1]
                if masked:
                    term = jnp.where(run >= offset, term, 0.0)
                total = total + term
            out_ref[pl.ds(at, step)] = total.astype(out_ref.dtype)

        short = short_ref[i] != 0

        @pl.when(short)
        def _():
            summed(True)

        @pl.when(jnp.logical_not(short))
        def _():
            summed(False)


def convolve(part, linear_part, gate_part, halo, taps, runs, short, after):
    rows = linear_part.shape[0] // 2
    width = linear_part.shape[1]
    back = rows // HALO
    block = lambda of: pl.BlockSpec((rows, LANES), of)
    return pl.pallas_call(
        functools.partial(conv_kernel, taps.shape[0]),
        out_shape=jax.ShapeDtypeStruct((rows, width), jnp.bfloat16),
        grid_spec=pltpu.PrefetchScalarGridSpec(
            num_scalar_prefetch=1,
            grid=(width // LANES,),
            in_specs=[
                block(lambda c, part: (part[0], c)),
                block(lambda c, part: (part[0], c)),
                pl.BlockSpec((HALO, LANES), lambda c, part: (part[0] * back - part[0], c)),
                pl.BlockSpec((HALO, LANES), lambda c, part: (part[0] * back - part[0], c)),
                pl.BlockSpec((HALO, LANES), lambda c, part: (0, c)),
                pl.BlockSpec((taps.shape[0], LANES), lambda c, part: (0, c)),
                block(lambda c, part: (0, 0)),
                pl.BlockSpec(memory_space=pltpu.SMEM),
                *[pl.BlockSpec(memory_space=pl.ANY) for _ in after],
            ],
            out_specs=block(lambda c, part: (0, c)),
            scratch_shapes=[pltpu.VMEM((HALO + rows, LANES), jnp.float32)],
        ),
        cost_estimate=pl.CostEstimate(
            flops=rows * width * taps.shape[0] * 12, bytes_accessed=rows * width * 6, transcendentals=0
        ),
        compiler_params=pltpu.CompilerParams(dimension_semantics=("arbitrary",)),
        name="convolve",
    )(part, linear_part, gate_part, linear_part, gate_part, halo, taps, runs, short, *after)


def row_norm(values):
    width = values.shape[1]
    mean = jnp.sum(values, 1, keepdims=True) * (1.0 / width)
    square = jnp.sum(values * values, 1, keepdims=True) * (1.0 / width)
    return (values - mean) * lax.rsqrt(square - mean * mean + EPSILON)


def project_kernel(own_ref, came_ref, own_gain_ref, came_gain_ref, w_own_ref, w_came_ref, residual_ref, gain_ref, *refs):
    out_ref = refs[-1]
    own = own_ref[...].astype(jnp.float32)
    came = came_ref[...].astype(jnp.float32)
    width = own.shape[1] + came.shape[1]
    mean = (jnp.sum(own, 1, keepdims=True) + jnp.sum(came, 1, keepdims=True)) * (1.0 / width)
    square = (
        jnp.sum(own * own, 1, keepdims=True) + jnp.sum(came * came, 1, keepdims=True)
    ) * (1.0 / width)
    scale = lax.rsqrt(square - mean * mean + EPSILON)
    own = jax.nn.silu((own - mean) * scale * own_gain_ref[...]).astype(jnp.bfloat16)
    came = jax.nn.silu((came - mean) * scale * came_gain_ref[...]).astype(jnp.bfloat16)
    projected = jnp.dot(own, w_own_ref[...], preferred_element_type=jnp.float32) + jnp.dot(
        came, w_came_ref[...], preferred_element_type=jnp.float32
    )
    mixed = RESIDUAL_SCALE * residual_ref[...].astype(jnp.float32) + projected
    out_ref[...] = (row_norm(mixed) * gain_ref[...]).astype(out_ref.dtype)


def project(first, count, own, came, own_gain, came_gain, w_own, w_came, residual, gain, before):
    total_rows, width = residual.shape
    half = own.shape[1]
    rows = min(count, 256)
    start = first // rows
    whole = lambda shape: pl.BlockSpec(shape, lambda r: (0, 0))
    here = lambda columns: pl.BlockSpec((rows, columns), lambda r: (r + start, 0))
    in_specs = [
        here(half),
        here(half),
        whole((1, half)),
        whole((1, half)),
        whole((half, width)),
        whole((half, width)),
        here(width),
        whole((1, width)),
    ]
    operands = [own, came, own_gain, came_gain, w_own, w_came, residual, gain]
    if before is not None:
        in_specs.append(pl.BlockSpec(memory_space=pl.ANY))
        operands.append(before)
    return pl.pallas_call(
        project_kernel,
        out_shape=jax.ShapeDtypeStruct((total_rows, width), jnp.bfloat16),
        grid=(count // rows,),
        in_specs=in_specs,
        out_specs=here(width),
        input_output_aliases={} if before is None else {8: 0},
        cost_estimate=pl.CostEstimate(
            flops=2 * count * width * width, bytes_accessed=4 * half * width + 6 * count * width, transcendentals=0
        ),
        compiler_params=pltpu.CompilerParams(dimension_semantics=("arbitrary",)),
        name="project",
    )(*operands)


def experts_kernel(group, piece, has_start, later, start_at, x_ref, table_ref, w_ref, *refs):
    start_ref = refs[0] if has_start else None
    out_ref, total, begun, in_sem, out_sem = refs[has_start + later :]
    rows, width = x_ref.shape
    step = pl.program_id(0)
    last = pl.num_programs(0) - 1
    tile = min(rows, 512)
    wide = 2 * piece
    kept = out_ref.dtype == jnp.float32
    started = lambda: pltpu.make_async_copy(start_ref.at[pl.ds(start_at, rows)], begun, in_sem)

    def sent(i):
        at = pl.ds(pl.multiple_of(i * tile, tile), tile)
        return pltpu.make_async_copy(total.at[at], out_ref.at[at], out_sem.at[i])

    @pl.when(step == 0)
    def _():
        if has_start:
            started().start()
        total[...] = jnp.zeros_like(total)

    @pl.when(step == last)
    def _():
        if has_start:
            started().wait()

    @pl.loop(0, rows // tile)
    def _(i):
        at = pl.ds(pl.multiple_of(i * tile, tile), tile)
        x = x_ref[at]
        table = table_ref[at]
        hidden = []
        for member in range(group):
            both = jnp.dot(x, w_ref[member, :width], preferred_element_type=jnp.float32)
            gate, up = both[:, :piece], both[:, piece:]
            weight = column_of(table, step * group + member)
            hidden.append((jax.nn.silu(gate) * up * weight).astype(jnp.bfloat16))
        hidden = jnp.concatenate(hidden, 1)
        for block in range(width // wide):
            low = width + block * piece
            down = jnp.concatenate([w_ref[member, low : low + piece] for member in range(group)], 0)
            columns = slice(block * wide, (block + 1) * wide)
            total[at, columns] += jnp.dot(hidden, down, preferred_element_type=jnp.float32)

        @pl.when(step == last)
        def _():
            result = total[at] + begun[at] if has_start else total[at]
            if kept:
                total[at] = result
                sent(i).start()
            else:
                out_ref[at] = result.astype(out_ref.dtype)

    if kept:

        @pl.when(step == last)
        def _():
            for i in range(rows // tile):
                sent(i).wait()


def experts(at, x, table, weights, start, dtype, after=()):
    first, count = at
    width = x.shape[1]
    experts_all, depth, wide = weights.shape
    piece = wide // 2
    group = 4 if experts_all % 4 == 0 else experts_all
    here = first // count
    anywhere = pl.BlockSpec(memory_space=pl.ANY)
    in_specs = [
        pl.BlockSpec((count, width), lambda e: (here, 0)),
        pl.BlockSpec((count, LANES), lambda e: (here, 0)),
        pl.BlockSpec((group, depth, wide), lambda e: (e, 0, 0)),
    ]
    operands = [x, table, weights]
    if start is not None:
        operands.append(start)
    operands.extend(after)
    in_specs.extend([anywhere] * (len(operands) - 3))
    kept = dtype == jnp.float32
    return pl.pallas_call(
        functools.partial(experts_kernel, group, piece, start is not None, len(after), first),
        out_shape=jax.ShapeDtypeStruct((count, width), dtype),
        grid=(experts_all // group,),
        in_specs=in_specs,
        out_specs=anywhere if kept else pl.BlockSpec((count, width), lambda e: (0, 0)),
        scratch_shapes=[
            pltpu.VMEM((count, width), jnp.float32),
            pltpu.VMEM((count if start is not None else 8, width), jnp.float32),
            pltpu.SemaphoreType.DMA,
            pltpu.SemaphoreType.DMA((max(count // 512, 1),)),
        ],
        cost_estimate=pl.CostEstimate(
            flops=2 * count * experts_all * depth * wide,
            bytes_accessed=2 * experts_all * depth * wide + 8 * count * width,
            transcendentals=0,
        ),
        compiler_params=pltpu.CompilerParams(
            dimension_semantics=("arbitrary",), vmem_limit_bytes=56 * 1024 * 1024
        ),
        name="experts",
    )(*operands)


def finish_kernel(normed_ref, routed_ref, came_ref, gain_ref, *refs):
    mixed = RESIDUAL_SCALE * normed_ref[...].astype(jnp.float32) + routed_ref[...]
    mixed = mixed + came_ref[...].astype(jnp.float32)
    refs[-1][...] = (row_norm(mixed) * gain_ref[...]).astype(jnp.bfloat16)


def finish(first, normed, routed, came, gain, before):
    rows, width = normed.shape
    count = came.shape[0]
    tile = 128
    start = first // tile
    here = pl.BlockSpec((tile, width), lambda r: (r + start, 0))
    in_specs = [here, here, pl.BlockSpec((tile, width), lambda r: (r, 0)), pl.BlockSpec((1, width), lambda r: (0, 0))]
    operands = [normed, routed, came, gain]
    if before is not None:
        in_specs.append(pl.BlockSpec(memory_space=pl.ANY))
        operands.append(before)
    return pl.pallas_call(
        finish_kernel,
        out_shape=jax.ShapeDtypeStruct((rows, width), jnp.bfloat16),
        grid=(count // tile,),
        in_specs=in_specs,
        out_specs=here,
        input_output_aliases={} if before is None else {4: 0},
        cost_estimate=pl.CostEstimate(
            flops=10 * count * width, bytes_accessed=14 * count * width, transcendentals=0
        ),
        compiler_params=pltpu.CompilerParams(dimension_semantics=("arbitrary",)),
        name="finish",
    )(*operands)


def packed(gate, up, down, low):
    width = gate.shape[0]
    blocks = width // (2 * PIECE)
    both = jnp.concatenate(
        [lax.dynamic_slice_in_dim(gate, low, PIECE, 1), lax.dynamic_slice_in_dim(up, low, PIECE, 1)], 1
    )
    below = lax.dynamic_slice_in_dim(down, low, PIECE, 0)
    below = below.reshape(PIECE, blocks, 2 * PIECE).transpose(1, 0, 2).reshape(blocks * PIECE, 2 * PIECE)
    return jnp.concatenate([both, below], 0)[None]


def swapped(block, axis):
    return lax.ppermute(block, axis, [(i, i ^ 1) for i in range(lax.axis_size(axis))])


def weight_table(names, weights):
    lanes = jnp.arange(LANES, dtype=jnp.float32)[None, :]
    return sum(
        jnp.where(names[k][:, None] == lanes, weights[k][:, None], 0.0) for k in range(names.shape[0])
    )


def shards_split(
    linear_part,
    gate_part,
    kernel_taps,
    channel_gain,
    output_weight,
    residual,
    mix_gain,
    documents,
    expert_ids,
    route_weights,
    expert_gate,
    expert_up,
    expert_down,
    shared_gate,
    shared_up,
    shared_down,
    final_gain,
):
    mine = lax.axis_index("tp")
    other = 1 - mine
    reach = kernel_taps.shape[0] - 1
    length = linear_part.shape[0]
    rows, width = residual.shape
    half = width // 2
    chosen = expert_ids.shape[1]
    low = mine * (expert_gate.shape[2] // 2)

    pieces = [
        packed(expert_gate[0], expert_up[0], expert_down[0], low + at)
        for at in range(0, expert_gate.shape[2] // 2, PIECE)
    ]
    gathered = [lax.all_gather(piece, "sp", axis=0, tiled=True) for piece in pieces]

    last_gated = (
        linear_part[length - HALO :].astype(jnp.float32)
        * jax.nn.sigmoid(gate_part[length - HALO :].astype(jnp.float32))
    ).astype(jnp.bfloat16)
    halo, halo_docs = passed_along((last_gated, documents[length - reach :]), "sp", 1)
    docs = jnp.concatenate([halo_docs, documents], 0)
    runs = sum(
        (docs[reach - offset : reach - offset + length] == documents).astype(jnp.int32)
        for offset in range(1, reach + 1)
    )
    short = (jnp.min(runs.reshape(length // 64, 64), 1) < reach).astype(jnp.int32)
    taps = kernel_taps.astype(jnp.float32)

    def conv_of(part, after=()):
        own_runs = lax.dynamic_slice_in_dim(runs, part * rows, rows)
        own_short = lax.dynamic_slice_in_dim(short, part * (rows // 64), rows // 64)
        return convolve(
            part[None],
            linear_part,
            gate_part,
            halo,
            taps,
            jnp.broadcast_to(own_runs[:, None], (rows, LANES)),
            own_short,
            after,
        )

    odd = lax.axis_index("sp") % 2
    quarter = half // 2
    fetched = swapped(lax.dynamic_slice_in_dim(output_weight, odd * quarter, quarter, 0), "tp")
    theirs = conv_of(other)
    came = swapped(theirs, "tp")
    own = conv_of(mine, (theirs,))
    fetched, own = lax.optimization_barrier((fetched, own))
    beside = swapped(fetched, "sp")
    w_came = jnp.concatenate([jnp.where(odd == 0, fetched, beside), jnp.where(odd == 0, beside, fetched)], 0)

    gain = channel_gain[None, :]
    own_gain = lax.dynamic_slice_in_dim(gain, mine * half, half, 1)
    came_gain = lax.dynamic_slice_in_dim(gain, other * half, half, 1)
    named = jnp.concatenate([expert_ids.T.astype(jnp.float32), route_weights.T], 0)
    named_there = swapped(named, "tp")
    table = weight_table(named[:chosen], named[chosen:])
    table_there = weight_table(named_there[:chosen], named_there[chosen:])

    part = rows // 2
    gains = mix_gain[None, :]
    normed, there = None, []
    for at in (0, part):
        normed = project(
            at, part, own, came, own_gain, came_gain, output_weight, w_came, residual, gains, normed
        )
        there.append(swapped(lax.slice_in_dim(normed, at, at + part), "tp"))

    common = (
        jax.nn.silu(jnp.dot(normed, shared_gate, preferred_element_type=jnp.float32))
        * jnp.dot(normed, shared_up, preferred_element_type=jnp.float32)
    ).astype(jnp.bfloat16)
    shared_out = jnp.dot(common, shared_down, preferred_element_type=jnp.float32)

    here_sum = experts((0, rows), normed, table, gathered[0], shared_out, jnp.float32)
    there_sums = [
        experts((0, part), there[k], table_there[k * part : (k + 1) * part], gathered[0], None, jnp.float32, (here_sum,))
        for k in range(2)
    ]
    waited = (here_sum, *there_sums)
    returned = []
    for first in range(0, rows, part // 2):
        k, at = divmod(first, part)
        count = part // 2
        done = experts(
            (at, count),
            there[k],
            table_there[k * part : (k + 1) * part],
            gathered[1],
            there_sums[k],
            jnp.bfloat16,
            waited,
        )
        returned.append(swapped(done, "tp"))
    routed = experts((0, rows), normed, table, gathered[1], here_sum, jnp.float32, waited)
    out, at = None, 0
    for block in returned:
        out = finish(at, normed, routed, block, final_gain[None, :], out)
        at += block.shape[0]
    return out


def shards(*arguments):
    linear_part, kernel_taps, residual, expert_gate = [arguments[at] for at in (0, 2, 5, 10)]
    splits = (
        lax.axis_size("tp") == 2
        and lax.axis_size("sp") % 4 == 0
        and expert_gate.shape[0] == 1
        and expert_gate.shape[2] == 4 * PIECE
        and residual.shape[0] % 1024 == 0
        and residual.shape[1] % 1024 == 0
        and kernel_taps.shape[0] <= HALO
    )
    return shards_split(*arguments) if splits else shards_any(*arguments)


def solution(mesh):
    return jax.shard_map(
        shards,
        mesh=mesh,
        in_specs=(
            P("sp", "tp"),
            P("sp", "tp"),
            P(None, "tp"),
            P(),
            P("tp", None),
            P(("sp", "tp"), None),
            P(),
            P("sp"),
            P(("sp", "tp"), None),
            P(("sp", "tp"), None),
            P("sp", None, None),
            P("sp", None, None),
            P("sp", None, None),
            P(),
            P(),
            P(),
            P(),
        ),
        out_specs=P(("sp", "tp"), None),
        check_vma=False,
    )
```
